512 devices in a mesh: sp: 32 (over z, core), tp: 16 (over y, x).
Axes of the slice: x: 4, y: 4, z: 16, core: 2. Of those that a mesh axis runs over, the one named last changes fastest.
Arguments:
- stream: bfloat16 [2048, 4096], P('tp', 'sp')
- values_in: bfloat16 [1024, 4096], P('tp', 'sp'), may hold values from -6 to 6
- in_gate: bfloat16 [1024, 4096], P('tp', 'sp'), may hold values from -6 to 6
- out_gate: bfloat16 [1024, 4096], P('tp', 'sp'), may hold values from -6 to 6
- documents: int32 [4096], P('sp'), may hold values from 0 to 63, never falling along the last dimension, each value on 1 to 256 neighbouring positions
- conv_taps: float32 [3, 1024], P(None, 'tp'), may hold values from -3.5 to 3.5
- head_gain: float32 [1024], P('tp'), may hold values from 0.1 to 1.9
- mix_weight: bfloat16 [1024, 2048], P('tp'), may hold values from -0.25 to 0.25
- norm_gain: float32 [2048], P('tp'), may hold values from 0.1 to 1.9
- routes: int32 [4096, 4], P('sp'), may hold values from 0 to 31, all different within a row; in each aligned block of 128 rows (0 to 127, 128 to 255, ...) at most 24 rows name the same one
- route_weight: float32 [4096, 4], P('sp'), may hold values from 0.2 to 1
- expert_gate: bfloat16 [32, 2048, 2048], P('sp', None, 'tp'), may hold values from -0.125 to 0.125
- expert_up: bfloat16 [32, 2048, 2048], P('sp', None, 'tp'), may hold values from -0.125 to 0.125
- expert_down: bfloat16 [32, 2048, 2048], P('sp', None, 'tp'), may hold values from -0.125 to 0.125
- shared_gate: bfloat16 [2048, 2048], P(None, 'tp'), may hold values from -0.125 to 0.125
- shared_up: bfloat16 [2048, 2048], P(None, 'tp'), may hold values from -0.125 to 0.125
- shared_down: bfloat16 [2048, 2048], P('tp'), may hold values from -0.1875 to 0.1875
Outputs:
- layer_out: bfloat16 [2048, 4096], P('tp', 'sp')
The draws below stay inside these ranges and needn't reach their ends.
Inputs may be any that keep to these rules, and one draw needn't show every extreme that they name: `routes`: each row names 4 different experts. In each aligned block of 128 rows no expert is named by more than 24 rows, a bound that some block reaches. `documents`: document numbers never fall along the positions; each document has 1 to 256 positions, and one has exactly that many.
All inputs are finite; a program needn't handle non-finite values.
Results may differ from the reference program's by a relative error of at most 0.015.
Values may be sent and summed in bfloat16 or wider, within the bound.
No kernel may reach another device: no remote copies, remote signals or barrier semaphores. Data moves between devices by JAX's collectives and lax.ppermute only.
A program may use at most 64 MiB of HBM per device.

```python
import math
import jax
import jax.numpy as jnp
import numpy as np
from jax import lax

D = 2048
HEADS = 16
HEAD = 64
CW = 1024
FE = 2048
FS = 2048
TOP_K = 4
TOK_DEV = 128
TOKENS = 4096
EXPERTS = 32
CAP = 24
N_SP = 32
N_TP = 16


def draw_stream(key, part):
    first = jax.random.fold_in(jax.random.fold_in(key, 11), 0)
    feature_scale = 0.5 * 4.0 ** (jnp.arange(D, dtype=jnp.float32) / D)
    base = jax.random.normal(first, (D, TOKENS), jnp.float32)
    return (base * feature_scale[:, None]).astype(jnp.bfloat16)


def with_spikes(entries, key, source, target, blocks, factor):
    owner, partner = [(jnp.arange(entries.shape[position]) // (entries.shape[position] // blocks)).reshape([-1 if axis == position else 1 for axis in range(entries.ndim)]) for position in (source, target)]
    chosen = jax.random.permutation(key, blocks)[partner]
    strong = (owner == chosen) | (owner == (partner + blocks // 2) % blocks)
    return jnp.where(strong, factor * entries, entries)


def steps_of(own_key, shape, pieces, low, high):
    factor_of = 1.0
    for dim, blocks in pieces:
        heights = jax.random.uniform(jax.random.fold_in(jax.random.fold_in(own_key, 6), dim), (blocks,), jnp.float32, low / len(pieces), high / len(pieces))
        factor_of = factor_of * jnp.repeat(jnp.exp(heights), shape[dim] // blocks).reshape((-1,) + (1,) * (len(shape) - 1 - dim))
    return factor_of


def profile(number_of, total, reach, slope):
    weights = [(1 << 20) // math.isqrt(rank ** slope) + 1 for rank in range(2, number_of + 1)]
    spare, counts = total - reach - (number_of - 1), [1] * (number_of - 1)
    while spare > 0:
        free = [i for i in range(number_of - 1) if counts[i] < reach]
        pool, budget = sum([weights[i] for i in free]), spare
        for i in free:
            addition = min(reach - counts[i], max(1, budget * weights[i] // pool), spare)
            counts[i] = counts[i] + addition
            spare = spare - addition
    return np.array([reach] + counts)


def uneven_parts(own_key, number_of, total, most, lean):
    if number_of == 2:
        one = jax.random.randint(own_key, (), max(1, total - most), min(most, total - 1) + 1)
        return jnp.stack([one, total - one])
    lengths = jnp.asarray(profile(number_of, total, most, lean), jnp.int32)
    twos = (number_of - 1) // 2
    donor, receiver = lengths[1:1 + 2 * twos:2], lengths[2:2 + 2 * twos:2]
    room = jnp.minimum(donor - 1, most - receiver)
    passed = jax.random.randint(jax.random.fold_in(own_key, 1), (twos,), 0, 1 << 20) % (room + 1)
    lengths = lengths.at[1:1 + 2 * twos:2].set(donor - passed).at[2:2 + 2 * twos:2].set(receiver + passed)
    return lengths[jax.random.permutation(jax.random.fold_in(own_key, 2), number_of)]


def deal_out(stream_key, own, number, rows, amount, top, reach, lean):
    ranking = jax.random.permutation(stream_key, amount)
    heavy_load, usual = portions_of(amount, rows * top, reach, lean, True), portions_of(amount, rows * top, reach, lean, False)
    places = jnp.arange(amount)

    def named(lengths, turn):
        used = int((lengths > 0).sum())
        fixed = max(1, used // 4)
        passed = fixed + (places - fixed + turn * (used - fixed)) % max(1, amount - fixed)
        return jnp.zeros((amount,), jnp.int32).at[ranking[jnp.where(places < fixed, places, passed)]].set(jnp.asarray(lengths, jnp.int32))

    lengths = jnp.where(number % 4 == 0, named(heavy_load, number // 4), named(usual, number - number // 4 - 1))
    mixed = jax.random.permutation(jax.random.fold_in(own, 3), amount)
    source_of, taker = mixed[0:amount // 2 * 2:2], mixed[1:amount // 2 * 2:2]
    room = jnp.minimum(lengths[source_of] - 1, reach - lengths[taker]) // 2
    room = jnp.where((source_of == ranking[0]) | (taker == ranking[0]) | (lengths[taker] == 0), 0, jnp.maximum(room, 0))
    passed = jax.random.randint(jax.random.fold_in(own, 4), (amount // 2,), 0, 1 << 20) % (room + 1)
    lengths = lengths.at[source_of].add(-passed).at[taker].add(passed)
    items = jnp.searchsorted(jnp.cumsum(lengths), jnp.arange(rows * top), side="right").astype(jnp.int32)
    listing = items.reshape(top, rows).T
    listing = listing[jax.random.permutation(jax.random.fold_in(own, 1), rows)]
    turn = jax.random.randint(jax.random.fold_in(own, 2), (rows, 1), 0, top)
    return jnp.take_along_axis(listing, (jnp.arange(top)[None, :] + turn) % top, axis=1)


def portions_of(amount, total, bound, skew, full):
    loads = [(1 << 20) // math.isqrt(standing ** skew) + 1 for standing in range(1, amount + 1)]
    largest = bound if full else min(bound, max(-(-total // amount), total * loads[0] // sum(loads)))
    least = 1 if total - largest >= amount - 1 else 0
    given, rest = [largest] + [least] * (amount - 1), total - largest - least * (amount - 1)
    while rest > 0:
        movable = [i for i in range(1, amount) if given[i] < largest] or [i for i in range(1, amount) if given[i] < bound]
        mass, budget = sum([loads[i] for i in movable]), rest
        for i in movable:
            more = min(bound - given[i], max(1, budget * loads[i] // mass), rest)
            given[i] = given[i] + more
            rest = rest - more
    return np.array(given)


def noise(own_key, extent, scale, bound, cuts=(), kind=jnp.bfloat16):
    array = jax.random.normal(own_key, extent, jnp.float32) * scale
    if len(cuts) > 0:
        array = steps_of(own_key, extent, cuts, -0.22, 0.18) * array
    return jnp.clip(array, min=-bound, max=bound).astype(kind)


def bell_draw_with(own_key, dims, scale, most, cuts, heavy, kind=jnp.bfloat16):
    result = scale * jax.random.normal(own_key, dims, jnp.float32)
    if cuts:
        result = result * steps_of(own_key, dims, cuts, -0.22, 0.18)
    return jnp.clip(with_spikes(result, jax.random.fold_in(own_key, 3), *heavy), -most, most).astype(kind)


def setup_inputs(seed: int = 0) -> dict:
    seeds = jax.random.split(jax.random.key(seed), 18)
    stream = draw_stream(jax.random.fold_in(seeds[17], 71), 0)
    values_in = noise(seeds[1], (CW, TOKENS), 1.0, 6.0, ((0, 16), (1, 32)))
    in_gate = noise(seeds[2], (CW, TOKENS), 1.0, 6.0, ((0, 16), (1, 32)))
    out_gate = noise(seeds[3], (CW, TOKENS), 1.0, 6.0, ((0, 16), (1, 32)))
    documents = jnp.searchsorted(jnp.cumsum(uneven_parts(seeds[4], 2 * N_SP, TOKENS, 2 * TOK_DEV, 1)), jnp.arange(TOKENS), side="right").astype(jnp.int32)
    conv_taps = noise(seeds[5], (3, CW), 3 ** -0.5, 3.5, ((1, 16),), jnp.float32)
    head_gain = jnp.clip(1.0 + 0.18 * jax.random.normal(seeds[6], (CW,), jnp.float32), 0.1, 1.9)
    mix_weight = bell_draw_with(seeds[7], (CW, D), CW ** -0.5, 0.25, ((0, 16),), (0, 1, 16, 2.0))
    norm_gain = jnp.clip(1.0 + 0.18 * jax.random.normal(seeds[8], (D,), jnp.float32), 0.1, 1.9)
    routes_keys = jax.random.split(jax.random.fold_in(seeds[9], 1), TOKENS // TOK_DEV)
    routes_turns = jax.random.permutation(jax.random.fold_in(seeds[9], 3), TOKENS // TOK_DEV)
    routes = jax.vmap(lambda own, number: deal_out(jax.random.fold_in(seeds[9], 2), own, number, TOK_DEV, EXPERTS, TOP_K, CAP, 1))(routes_keys, routes_turns).reshape((TOKENS, TOP_K))
    route_weight = jnp.clip(0.2 + 0.8 * jax.random.uniform(seeds[10], (TOKENS, TOP_K), jnp.float32) ** steps_of(seeds[10], (TOKENS, TOP_K), ((0, 32),), -0.2, 0.2), 0.2, 1.0)
    expert_gate = noise(seeds[11], (EXPERTS, D, FE), D ** -0.5, 0.125, ((0, 32), (2, 16)))
    expert_up = noise(seeds[12], (EXPERTS, D, FE), D ** -0.5, 0.125, ((0, 32), (2, 16)))
    expert_down = noise(seeds[13], (EXPERTS, FE, D), FE ** -0.5, 0.125, ((0, 32), (2, 16)))
    shared_gate = noise(seeds[14], (D, FS), D ** -0.5, 0.125, ((1, 16),))
    shared_up = noise(seeds[15], (D, FS), D ** -0.5, 0.125, ((1, 16),))
    shared_down = bell_draw_with(seeds[16], (FS, D), FS ** -0.5, 0.1875, ((0, 16),), (0, 1, 16, 2.0))
    return {"stream": stream, "values_in": values_in, "in_gate": in_gate, "out_gate": out_gate, "documents": documents, "conv_taps": conv_taps, "head_gain": head_gain, "mix_weight": mix_weight, "norm_gain": norm_gain, "routes": routes, "route_weight": route_weight, "expert_gate": expert_gate, "expert_up": expert_up, "expert_down": expert_down, "shared_gate": shared_gate, "shared_up": shared_up, "shared_down": shared_down}


epsilon = 1e-06

def rounded(value):
    return lax.optimization_barrier(value.astype(jnp.bfloat16)).astype(jnp.float32)

def block_sum(left, right, parts):
    width = left.shape[1] // parts
    running = jnp.zeros((left.shape[0], right.shape[1]), jnp.float32)
    for block in range(parts):
        term = jnp.dot(left[:, block * width:(block + 1) * width], right[block * width:(block + 1) * width], preferred_element_type=jnp.float32)
        running = running + rounded(term)
    return running

def reference(stream, values_in, in_gate, out_gate, documents, conv_taps, head_gain, mix_weight, norm_gain, routes, route_weight, expert_gate, expert_up, expert_down, shared_gate, shared_up, shared_down):
    product = values_in.astype(jnp.float32) * in_gate.astype(jnp.float32)
    length = product.shape[1]
    padded = jnp.pad(product, ((0, 0), (2, 0)))
    doc_ids = jnp.pad(documents, (2, 0), constant_values=-1)
    convolved = jnp.zeros(product.shape, jnp.float32)
    for offset in range(3):
        same_doc = (doc_ids[offset:offset + length] == documents).astype(jnp.float32)
        convolved = convolved + conv_taps[offset][:, None] * padded[:, offset:offset + length] * same_doc[None, :]
    mixed = out_gate.astype(jnp.float32) * convolved
    heads = mixed.reshape(HEADS, HEAD, length)
    heads = heads * lax.rsqrt(lax.optimization_barrier(jnp.mean(heads * heads, axis=1, keepdims=True)) + epsilon)
    normed_heads = (heads.reshape(CW, length) * head_gain[:, None]).astype(jnp.bfloat16)
    mixer = block_sum(normed_heads.T, mix_weight, N_TP)
    hidden_state = stream.astype(jnp.float32).T + mixer
    normed = (hidden_state * lax.rsqrt(lax.optimization_barrier(jnp.mean(hidden_state * hidden_state, axis=1, keepdims=True)) + epsilon) * norm_gain[None, :]).astype(jnp.bfloat16)
    shared_mid = (jax.nn.silu(jnp.dot(normed, shared_gate, preferred_element_type=jnp.float32)) * jnp.dot(normed, shared_up, preferred_element_type=jnp.float32)).astype(jnp.bfloat16)
    shared = block_sum(shared_mid, shared_down, N_TP)
    groups = TOKENS // TOK_DEV
    flat_routes = routes.reshape(groups, TOK_DEV * TOP_K)
    onehot = (flat_routes[:, :, None] == jnp.arange(EXPERTS, dtype=jnp.int32)[None, None, :]).astype(jnp.int32)
    earlier = jnp.cumsum(onehot, axis=1) - onehot
    slot = lax.optimization_barrier(jnp.sum(earlier * onehot, axis=2))
    column = (jnp.arange(groups, dtype=jnp.int32)[:, None] * CAP + slot).reshape(-1).astype(jnp.int32)
    owner = (jnp.arange(TOKENS * TOP_K, dtype=jnp.int32) // TOP_K).astype(jnp.int32)
    chosen = flat_routes.reshape(-1)
    table = jnp.zeros((EXPERTS, groups * CAP), jnp.int32).at[chosen, column].set(owner)
    filled = jnp.zeros((EXPERTS, groups * CAP), jnp.bfloat16).at[chosen, column].set(1.0)

    def expert(number):
        rows = normed[table[number]] * filled[number][:, None]
        gate = jnp.dot(rows, expert_gate[number], preferred_element_type=jnp.float32)
        upward = jnp.dot(rows, expert_up[number], preferred_element_type=jnp.float32)
        middle = (jax.nn.silu(gate) * upward).astype(jnp.bfloat16)
        return jnp.dot(middle, expert_down[number], preferred_element_type=jnp.float32).astype(jnp.bfloat16)
    outputs = lax.map(expert, jnp.arange(EXPERTS, dtype=jnp.int32))
    picked = outputs[chosen, column].astype(jnp.float32).reshape(TOKENS, TOP_K, D)
    routed = lax.optimization_barrier(jnp.sum(picked * route_weight[:, :, None], axis=1))
    return (hidden_state + shared + routed).astype(jnp.bfloat16).T
```

```python
import jax
import jax.numpy as jnp
from jax import lax
from jax.sharding import Mesh
from jax.sharding import PartitionSpec as P

D = 2048
HEAD = 64
TP = ("ty", "tx")


epsilon = 1e-06


def shifted(x, axis, by, wrap):
    size = lax.axis_size(axis)
    pairs = [(i, (i + by) % size) for i in range(size) if wrap or 0 <= i + by < size]
    return lax.ppermute(x, axis, pairs)


def sum_at_owner(x, axis):
    pieces = x.reshape(lax.axis_size(axis), -1, x.shape[-1])
    arrived = lax.all_to_all(pieces, axis, split_axis=0, concat_axis=0, tiled=True)
    return arrived.astype(jnp.float32).sum(axis=0)


def from_everyone(x, axis):
    size = lax.axis_size(axis)
    return lax.all_to_all(jnp.broadcast_to(x[None], (size, *x.shape)), axis, 0, 0, tiled=True)


def contract_rows(left, right):
    return lax.dot_general(
        left, right, (((0,), (0,)), ((), ())), preferred_element_type=jnp.float32
    )


def three_terms(x):
    high = x.astype(jnp.bfloat16)
    rest = x - high.astype(jnp.float32)
    middle = rest.astype(jnp.bfloat16)
    low = (rest - middle.astype(jnp.float32)).astype(jnp.bfloat16)
    return [high, middle, low]


def local(
    stream,
    values_in,
    in_gate,
    out_gate,
    documents,
    conv_taps,
    head_gain,
    mix_weight,
    norm_gain,
    routes,
    route_weight,
    expert_gate,
    expert_up,
    expert_down,
    shared_gate,
    shared_up,
    shared_down,
):
    positions = stream.shape[1]
    feat_rows = stream.shape[0]
    sp_count = lax.axis_size("sp")
    parts = lax.axis_size("ty")
    top_count = routes.shape[1]
    capacity = 3 * positions * top_count // (2 * sp_count)
    share = capacity // parts
    row = lax.axis_index("ty")
    col = lax.axis_index("tx")

    packed = jnp.stack([expert_gate[0], expert_up[0], expert_down[0]])
    packed = packed.reshape(3, parts, 2, -1, feat_rows, feat_rows)
    packed = packed.transpose(2, 0, 3, 1, 4, 5).reshape(2, 3, D // 2, feat_rows)
    before_w = shifted(packed, "ty", 1, True)
    after_w = shifted(packed, "ty", -1, True)
    far_first = shifted(before_w[0], "ty", 1, True)
    far_second = shifted(after_w[1], "ty", -1, True)
    cycle = [
        (packed[0], packed[1]),
        (after_w[0], after_w[1]),
        (far_first, far_second),
        (before_w[0], before_w[1]),
    ]

    def in_order(blocks):
        twice = jnp.concatenate([blocks, blocks], axis=0)
        return lax.dynamic_slice_in_dim(twice, (parts - row) % parts, parts, axis=0)

    tails = jnp.stack([values_in[:, -2:], in_gate[:, -2:]])
    before, before_docs = shifted((tails, documents[-2:]), "sp", 1, False)
    joined = jnp.concatenate([before, jnp.stack([values_in, in_gate])], axis=2).astype(jnp.float32)
    product = joined[0] * joined[1]
    doc_ids = jnp.concatenate([before_docs, documents])
    convolved = jnp.zeros((values_in.shape[0], positions), jnp.float32)
    for offset in range(3):
        same_doc = (doc_ids[offset : offset + positions] == documents).astype(jnp.float32)
        convolved = (
            convolved
            + conv_taps[offset][:, None]
            * product[:, offset : offset + positions]
            * same_doc[None, :]
        )
    mixed = out_gate.astype(jnp.float32) * convolved
    heads = mixed.reshape(-1, HEAD, positions)
    heads = heads * lax.rsqrt(jnp.mean(heads * heads, axis=1, keepdims=True) + epsilon)
    normed_heads = (heads.reshape(mixed.shape) * head_gain[:, None]).astype(jnp.bfloat16)
    mixer = sum_at_owner(contract_rows(mix_weight, normed_heads).astype(jnp.bfloat16), TP)
    hidden_state = stream.astype(jnp.float32) + mixer

    squares = three_terms(jnp.sum(hidden_state * hidden_state, axis=0, keepdims=True))
    scaled = (hidden_state * norm_gain[:, None]).astype(jnp.bfloat16)
    filler = jnp.zeros((13, positions), jnp.bfloat16)
    everyone = from_everyone(jnp.concatenate([scaled, *squares, filler]), TP)
    total = jnp.sum(everyone[:, feat_rows : feat_rows + 3].astype(jnp.float32), axis=(0, 1))
    inverse = lax.rsqrt(total / D + epsilon)
    full_rows = (everyone[:, :feat_rows].astype(jnp.float32) * inverse).astype(jnp.bfloat16)

    flat_routes = routes.reshape(-1)
    onehot = (flat_routes[:, None] == jnp.arange(sp_count, dtype=jnp.int32)[None, :]).astype(
        jnp.int32
    )
    earlier = jnp.cumsum(onehot, axis=0) - onehot
    slot = jnp.sum(earlier * onehot, axis=1)
    inside = (slot >= row * share) & (slot < (row + 1) * share)
    column = jnp.where(inside, flat_routes * share + slot - row * share, -1)
    slot_total = sp_count * share
    chosen = (column[:, None] == jnp.arange(slot_total, dtype=jnp.int32)[None, :]).reshape(
        positions, top_count, slot_total
    )
    dispatch = jnp.any(chosen, axis=1).astype(jnp.bfloat16)
    combine = jnp.sum(chosen.astype(jnp.float32) * route_weight[:, :, None], axis=1)

    by_col = full_rows.reshape(parts, -1, feat_rows, positions)
    mine = lax.dynamic_index_in_dim(by_col, col, 1, keepdims=False)
    sent = lax.dot_general(
        dispatch,
        mine.reshape(parts * feat_rows, positions),
        (((0,), (1,)), ((), ())),
        preferred_element_type=jnp.float32,
    ).astype(jnp.bfloat16)
    arrived = lax.all_to_all(
        sent.reshape(sp_count, share * parts, feat_rows), "sp", split_axis=0, concat_axis=0, tiled=True
    )

    rows_full = full_rows.reshape(D, positions)
    shared_mid = (
        jax.nn.silu(contract_rows(shared_gate, rows_full)) * contract_rows(shared_up, rows_full)
    ).astype(jnp.bfloat16)
    shared = contract_rows(shared_down, shared_mid)

    def times(x, which, block):
        half = x.shape[0] // 2

        def part(k):
            w = cycle[block][k][which].reshape(half, -1, feat_rows)
            return lax.dot_general(
                x[k * half : (k + 1) * half],
                w,
                (((0, 2), (0, 1)), ((), ())),
                preferred_element_type=jnp.float32,
            )

        return part(0) + part(1)

    block_rows = lax.all_gather(arrived.reshape(slot_total, parts * feat_rows), "tx", axis=0)
    expert_mid = in_order(
        jnp.stack(
            [
                (jax.nn.silu(times(block_rows, 0, n)) * times(block_rows, 1, n)).astype(jnp.bfloat16)
                for n in range(parts)
            ]
        )
    )
    expert_mid = expert_mid.transpose(1, 0, 2).reshape(slot_total, parts * feat_rows)
    all_mid = lax.all_gather(expert_mid, "tx", axis=0)
    summed = in_order(
        jnp.stack([times(all_mid, 2, n).astype(jnp.bfloat16) for n in range(parts)])
    )
    summed = summed.transpose(1, 0, 2).reshape(sp_count, share * parts, feat_rows)
    returned = lax.all_to_all(summed, "sp", split_axis=0, concat_axis=0, tiled=True)
    routed = lax.dot_general(
        returned.reshape(slot_total, parts * feat_rows).astype(jnp.float32),
        combine,
        (((0,), (1,)), ((), ())),
        precision=lax.Precision.HIGHEST,
        preferred_element_type=jnp.float32,
    )
    here = (jnp.arange(lax.axis_size("tx")) == col).astype(jnp.float32)
    both = shared.reshape(parts, -1, feat_rows, positions) + (
        routed.reshape(parts, 1, feat_rows, positions) * here[None, :, None, None]
    )
    experts = sum_at_owner(both.reshape(D, positions).astype(jnp.bfloat16), TP)
    return (hidden_state + experts).astype(jnp.bfloat16)


def solution(mesh):
    split = Mesh(mesh.devices.reshape(mesh.shape["sp"], 4, 4), ("sp", "ty", "tx"))
    in_specs = (
        P(TP, "sp"),
        P(TP, "sp"),
        P(TP, "sp"),
        P(TP, "sp"),
        P("sp"),
        P(None, TP),
        P(TP),
        P(TP, None),
        P(TP),
        P("sp", None),
        P("sp", None),
        P("sp", None, TP),
        P("sp", None, TP),
        P("sp", None, TP),
        P(None, TP),
        P(None, TP),
        P(TP, None),
    )
    out_specs = P(TP, "sp")
    return jax.shard_map(local, mesh=split, in_specs=in_specs, out_specs=out_specs, check_vma=False)
```
